32 devices in a mesh: sp: 8 (over z, x), tp: 4 (over y, core).
Axes of the slice: x: 2, y: 2, z: 4, core: 2. Of those that a mesh axis runs over, the one named last changes fastest.
Arguments:
- tokens: bfloat16 [2048, 4096], P(('sp', 'tp')), may hold values from -8 to 8, as said below
- q_weight: bfloat16 [4096, 4096], P('sp', 'tp'), may hold values from -0.09375 to 0.09375
- k_weight: bfloat16 [4096, 1024], P('sp', 'tp'), may hold values from -0.09375 to 0.09375
- v_weight: bfloat16 [4096, 1024], P('sp', 'tp'), may hold values from -0.09375 to 0.09375
- o_weight: bfloat16 [4096, 4096], P('tp', 'sp'), may hold values from -0.09375 to 0.09375
- q_gain: float32 [128], replicated, may hold values from 0.1 to 1.9
- k_gain: float32 [128], replicated, may hold values from 0.1 to 1.9
- out_gain: float32 [4096], replicated, may hold values from 0.1 to 1.9
Outputs:
- result: bfloat16 [2048, 4096], P(('sp', 'tp'))
The draws below stay inside these ranges and needn't reach their ends.
Inputs may be any that keep to these rules, and one draw needn't show every extreme that they name: tokens are random draws plus a smooth per-channel wave along the sequence, so that their mean differs between parts of the sequence.
All inputs are finite; a program needn't handle non-finite values.
Results may differ from the reference program's by a relative error of at most 0.02.
Values may be sent and summed in bfloat16 or wider, within the bound.
A program may use at most 128 MiB of HBM per device.

```python
import math
import jax
import jax.numpy as jnp
from jax import lax

D = 4096
HEADS = 32
KV_HEADS = 8
HEAD_DIM = 128
GRID_W = 64
SEQ = 2048


def draw_tokens(key, part):
    key_base, key_amp, key_phase = jax.random.split(key, 3)
    base = jnp.clip(jax.random.normal(key_base, (SEQ, D), jnp.float32), -5.0, 5.0)
    amplitude = 0.8 * jnp.clip(jax.random.normal(key_amp, (D,), jnp.float32), -2.5, 2.5)
    phases = jax.random.uniform(key_phase, (D,), jnp.float32, 0.0, 2.0 * math.pi)
    where = jnp.arange(SEQ, dtype=jnp.float32) / SEQ
    wave = amplitude[None, :] * jnp.cos(2.0 * math.pi * where[:, None] + phases[None, :])
    return (base + wave).astype(jnp.bfloat16)


def block_scale(stream_key, shape, shards, least, high):
    loudness, own = 1.0, jax.random.fold_in(stream_key, 6)
    for axis_at, shards_of in shards:
        heights = jnp.exp(jax.random.uniform(jax.random.fold_in(own, axis_at), (shards_of,), jnp.float32, least / len(shards), high / len(shards)))
        loudness = loudness * jnp.repeat(heights, shape[axis_at] // shards_of).reshape([-1 if axis == axis_at else 1 for axis in range(len(shape))])
    return loudness


def noise(rng, extent, width, bound, shards=(), kind=jnp.bfloat16):
    factor_of = block_scale(rng, extent, shards, -0.22, 0.18) if shards else 1.0
    values = jax.random.normal(rng, extent, jnp.float32) * width * factor_of
    return jnp.minimum(jnp.maximum(values, -bound), bound).astype(kind)


def setup_inputs(seed: int = 0) -> dict:
    key_list = jax.random.split(jax.random.key(seed), 9)
    tokens = draw_tokens(jax.random.fold_in(key_list[8], 71), 0)
    q_weight = noise(key_list[1], (D, HEADS * HEAD_DIM), D ** -0.5, 0.09375, ((0, 8), (1, 4)))
    k_weight = noise(key_list[2], (D, KV_HEADS * HEAD_DIM), D ** -0.5, 0.09375, ((0, 8), (1, 4)))
    v_weight = noise(key_list[3], (D, KV_HEADS * HEAD_DIM), D ** -0.5, 0.09375, ((0, 8), (1, 4)))
    o_weight = noise(key_list[4], (HEADS * HEAD_DIM, D), (HEADS * HEAD_DIM) ** -0.5, 0.09375, ((0, 4), (1, 8)))
    q_gain = jnp.clip(1.0 + 0.18 * jax.random.normal(key_list[5], (HEAD_DIM,), jnp.float32), 0.1, 1.9)
    k_gain = jnp.clip(1.0 + 0.18 * jax.random.normal(key_list[6], (HEAD_DIM,), jnp.float32), 0.1, 1.9)
    out_gain = jnp.clip(1.0 + 0.18 * jax.random.normal(key_list[7], (D,), jnp.float32), 0.1, 1.9)
    return dict(tokens=tokens, q_weight=q_weight, k_weight=k_weight, v_weight=v_weight, o_weight=o_weight, q_gain=q_gain, k_gain=k_gain, out_gain=out_gain)


EPS = 1e-06
THETA = 10000.0

def tables(positions, head_dim):
    quarter = head_dim // 4
    grid_row = (positions // GRID_W).astype(jnp.float32)
    grid_col = (positions % GRID_W).astype(jnp.float32)
    inv_freq = 1.0 / THETA ** (jnp.arange(quarter, dtype=jnp.float32) * 2.0 / (head_dim // 2))
    ang_row = grid_row[:, None] * inv_freq[None, :]
    ang_col = grid_col[:, None] * inv_freq[None, :]
    angles = jnp.concatenate([ang_row, ang_row, ang_col, ang_col], axis=-1)
    return (jnp.cos(angles), jnp.sin(angles))

def norm_rope(raw_proj, gain_vec, positions):
    head_dim = raw_proj.shape[-1]
    values = raw_proj.astype(jnp.float32)
    values = values * lax.rsqrt(lax.optimization_barrier(jnp.mean(values * values, axis=-1, keepdims=True)) + EPS) * gain_vec
    cosine, sine_vals = tables(positions, head_dim)
    halves = values.reshape(values.shape[:-1] + (2, 2, head_dim // 4))
    rotated = jnp.stack([-halves[..., 1, :], halves[..., 0, :]], axis=-2).reshape(values.shape)
    return values * cosine[:, None, :] + rotated * sine_vals[:, None, :]

def reference(tokens, q_weight, k_weight, v_weight, o_weight, q_gain, k_gain, out_gain):
    groups = HEADS // KV_HEADS
    positions = jnp.arange(SEQ, dtype=jnp.int32)
    q_proj = jnp.dot(tokens, q_weight, preferred_element_type=jnp.float32).astype(jnp.bfloat16)
    k_proj = jnp.dot(tokens, k_weight, preferred_element_type=jnp.float32).astype(jnp.bfloat16)
    v_proj = jnp.dot(tokens, v_weight, preferred_element_type=jnp.float32).astype(jnp.bfloat16)
    queries = norm_rope(q_proj.reshape(SEQ, HEADS, HEAD_DIM), q_gain, positions).astype(jnp.bfloat16)
    keys = norm_rope(k_proj.reshape(SEQ, KV_HEADS, HEAD_DIM), k_gain, positions).astype(jnp.bfloat16)
    keys_wide = keys.astype(jnp.float32)
    vals_wide = v_proj.reshape(SEQ, KV_HEADS, HEAD_DIM).astype(jnp.float32)
    score_scale = HEAD_DIM ** (-0.5)
    block = 128
    query_blocks = queries.reshape(SEQ // block, block, KV_HEADS, groups, HEAD_DIM)

    def attend(query_blk):
        scores = jnp.einsum('qkgd,tkd->kgqt', query_blk.astype(jnp.float32), keys_wide) * score_scale
        row_max = lax.optimization_barrier(jnp.max(scores, axis=-1, keepdims=True))
        probs = jnp.exp(scores - row_max)
        denom = lax.optimization_barrier(jnp.sum(probs, axis=-1))
        rounded = lax.optimization_barrier(probs.astype(jnp.bfloat16))
        numer = jnp.einsum('kgqt,tkd->kgqd', rounded.astype(jnp.float32), vals_wide)
        return (numer / denom[..., None]).transpose(2, 0, 1, 3)
    attended = lax.map(attend, query_blocks).reshape(SEQ, HEADS * HEAD_DIM).astype(jnp.bfloat16)
    mixed = jnp.dot(attended, o_weight, preferred_element_type=jnp.float32)
    normed = mixed * lax.rsqrt(lax.optimization_barrier(jnp.mean(mixed * mixed, axis=-1, keepdims=True)) + EPS) * out_gain
    return normed.astype(jnp.bfloat16)
```

```python
import functools

import jax
import jax.numpy as jnp
from jax import lax
from jax.experimental import pallas as pl
from jax.experimental.pallas import tpu as pltpu
from jax.sharding import PartitionSpec as P

GRID_W = 64


EPS = 1e-06
THETA = 10000.0


def tables(positions, head_dim):
    quarter = head_dim // 4
    grid_row = (positions // GRID_W).astype(jnp.float32)
    grid_col = (positions % GRID_W).astype(jnp.float32)
    inv_freq = 1.0 / THETA ** (jnp.arange(quarter, dtype=jnp.float32) * 2.0 / (head_dim // 2))
    ang_row = grid_row[:, None] * inv_freq[None, :]
    ang_col = grid_col[:, None] * inv_freq[None, :]
    angles = jnp.concatenate([ang_row, ang_row, ang_col, ang_col], axis=-1)
    return (jnp.cos(angles), jnp.sin(angles))


def norm_rope(raw_proj, gain_vec, positions):
    head_dim = raw_proj.shape[-1]
    values = raw_proj.astype(jnp.float32)
    values = values * lax.rsqrt(jnp.mean(values * values, axis=-1, keepdims=True) + EPS) * gain_vec
    cosine, sine_vals = tables(positions, head_dim)
    halves = values.reshape(values.shape[:-1] + (2, 2, head_dim // 4))
    rotated = jnp.stack([-halves[..., 1, :], halves[..., 0, :]], axis=-2).reshape(values.shape)
    return values * cosine[:, None, :] + rotated * sine_vals[:, None, :]


def on_device(tokens, q_weight, k_weight, v_weight, o_weight, q_gain, k_gain, out_gain):
    q_full, k_full, v_full, o_full = (
        lax.all_gather(q_weight, "sp", axis=0, tiled=True),
        lax.all_gather(k_weight, "sp", axis=0, tiled=True),
        lax.all_gather(v_weight, "sp", axis=0, tiled=True),
        lax.all_gather(o_weight, "sp", axis=1, tiled=True),
    )
    query_cols = q_full.shape[1]
    value_cols = k_full.shape[1]
    head_dim = q_gain.shape[0]
    local_kv = value_cols // head_dim
    groups = query_cols // value_cols

    def project(portion):
        return jnp.concatenate(
            [
                jnp.dot(portion, q_full, preferred_element_type=jnp.float32),
                jnp.dot(portion, k_full, preferred_element_type=jnp.float32),
                jnp.dot(portion, v_full, preferred_element_type=jnp.float32),
            ],
            axis=1,
        )

    projected = project(lax.all_gather(tokens, "tp", axis=0, tiled=True)).astype(jnp.bfloat16)
    tok_rows = projected.shape[0]
    positions = lax.axis_index("sp") * tok_rows + lax.iota(jnp.int32, tok_rows)
    queries = norm_rope(
        projected[:, :query_cols].reshape(tok_rows, local_kv * groups, head_dim), q_gain, positions
    )
    queries = queries.astype(jnp.bfloat16).reshape(tok_rows, local_kv, groups, head_dim)
    keys = norm_rope(
        projected[:, query_cols : query_cols + value_cols].reshape(tok_rows, local_kv, head_dim),
        k_gain,
        positions,
    )
    keys = keys.astype(jnp.bfloat16)
    values = projected[:, query_cols + value_cols :].reshape(tok_rows, local_kv, head_dim)
    score_scale = head_dim ** (-0.5)

    def absorb(state_in, key_blk, val_blk):
        run_max, run_sum, run_acc = state_in
        scores = (
            jnp.einsum("qkgd,tkd->kgqt", queries, key_blk, preferred_element_type=jnp.float32)
            * score_scale
        )
        new_max = jnp.maximum(run_max, jnp.max(scores, axis=-1))
        shrink = jnp.exp(run_max - new_max)
        probs_blk = jnp.exp(scores - new_max[..., None])
        run_sum = run_sum * shrink + jnp.sum(probs_blk, axis=-1)
        update = jnp.einsum(
            "kgqt,tkd->kgqd",
            probs_blk.astype(jnp.bfloat16),
            val_blk,
            preferred_element_type=jnp.float32,
        )
        run_acc = run_acc * shrink[..., None] + update
        return (new_max, run_sum, run_acc)

    def fold_keys(state_in, pieces):
        key_piece, val_piece = pieces
        row_count = key_piece.shape[0]
        width = 512 if row_count % 512 == 0 else row_count
        key_blocks = key_piece.reshape(row_count // width, width, local_kv, head_dim)
        val_blocks = val_piece.reshape(row_count // width, width, local_kv, head_dim)

        def scan_step(state_now, block_pair):
            return (absorb(state_now, block_pair[0], block_pair[1]), None)

        state_out, unused = lax.scan(scan_step, state_in, (key_blocks, val_blocks))
        return state_out

    initial = (
        jnp.full((local_kv, groups, tok_rows), -1e30, jnp.float32),
        jnp.zeros((local_kv, groups, tok_rows), jnp.float32),
        jnp.zeros((local_kv, groups, tok_rows, head_dim), jnp.float32),
    )
    run_max, run_sum, run_acc = fold_keys(
        initial,
        (
            lax.all_gather(keys, "sp", axis=0, tiled=True),
            lax.all_gather(values, "sp", axis=0, tiled=True),
        ),
    )
    attended = (
        (run_acc / run_sum[..., None])
        .transpose(2, 0, 1, 3)
        .reshape(tok_rows, query_cols)
        .astype(jnp.bfloat16)
    )

    def out_term():
        picked = lax.slice_in_dim(attended, 0, own_rows * lax.axis_size("tp"), axis=0)
        return jnp.dot(picked, o_full, preferred_element_type=jnp.float32)

    own_rows = tokens.shape[0]
    mixed = lax.psum_scatter(
        out_term().astype(jnp.bfloat16), "tp", scatter_dimension=0, tiled=True
    ).astype(jnp.float32)
    normed = mixed * lax.rsqrt(jnp.mean(mixed * mixed, axis=-1, keepdims=True) + EPS) * out_gain
    return normed.astype(jnp.bfloat16)


MESH = pl.DeviceIdType.MESH
F32, BF16 = jnp.float32, jnp.bfloat16
LOG2E = 1.4426950408889634


def sem_shapes(Z, X, Y, C, J):
    return {
        "t1": (Z,),
        "t2": (Y, Z),
        "t3": (C, Y, Z),
        "wkv": (X, 2),
        "wq": (X, J),
        "wo": (X,),
        "pkv": (Z,),
        "pq": (J, Z),
        "kz": (Z,),
        "kx": (X, Z),
        "at": (J, Z),
        "mc": (C, Z),
        "my": (Y, Z),
        "ft": (Z,),
    }


def fused_kernel(Z, X, Y, C, J, G, hd, names, *refs):
    (tok, wq, wk, wv, wo, qg, kg, og, cos, sin, out) = refs[:11]
    (T, WQX, WKX, WVX, WOX, PKV, RKV, AKV, PQ, RQ, AQ, KV, QB, AT, MB, MC, MS, MY, FS, FB) = refs[11:31]
    sems = {n: (refs[31 + 2 * i], refs[32 + 2 * i]) for i, n in enumerate(names)}

    sp, tp = lax.axis_index("sp"), lax.axis_index("tp")
    z, x = lax.div(sp, X), lax.rem(sp, X)
    y, c = lax.div(tp, C), lax.rem(tp, C)
    R, D = tok.shape
    TP = Y * C
    TR = TP * R
    Kx = wq.shape[0]
    Kz = Kx * X
    Gc = G * hd
    Kc = J * hd
    No = wo.shape[1]

    def up(v, d, n):
        return lax.rem(v + d, n)

    def dn(v, d, n):
        return lax.rem(v + n - d, n)

    def dev(zz, xx, yy, cc):
        return {"sp": zz * X + xx, "tp": yy * C + cc}

    def zdev(d):
        return dev(up(z, d, Z), x, y, c)

    def xdev(d):
        return dev(z, up(x, d, X), y, c)

    def ydev(d):
        return dev(z, x, up(y, d, Y), c)

    def cdev(d):
        return dev(z, x, y, up(c, d, C))

    sent = []

    def send(src, dst, name, idx, to):
        s, r = sems[name]
        cp = pltpu.make_async_remote_copy(
            src_ref=src, dst_ref=dst, send_sem=s.at[idx], recv_sem=r.at[idx],
            device_id=to, device_id_type=MESH,
        )
        cp.start()
        sent.append(cp)

    def recv(dst, name, idx):
        s, r = sems[name]
        pltpu.make_async_remote_copy(
            src_ref=dst, dst_ref=dst, send_sem=s.at[idx], recv_sem=r.at[idx],
            device_id=cdev(1), device_id_type=MESH,
        ).wait_recv()

    def cols(k, n):
        return pl.ds(pl.multiple_of(k * n, n), n)

    barrier = pltpu.get_barrier_semaphore()
    peers = [zdev(d) for d in range(1, Z)] + [xdev(d) for d in range(1, X)]
    peers += [ydev(d) for d in range(1, Y)] + [cdev(d) for d in range(1, C)]
    for p in peers:
        pl.semaphore_signal(barrier, inc=1, device_id=p, device_id_type=MESH)
    pl.semaphore_wait(barrier, len(peers))

    for d in range(1, Z):
        send(tok.at[:, cols(up(z, d, Z), Kz)], T.at[z, tp], "t1", (d,), zdev(d))
    for d in range(1, X):
        send(wk, WKX.at[d - 1], "wkv", (d, 0), xdev(d))
        send(wv, WVX.at[d - 1], "wkv", (d, 1), xdev(d))
        for j in range(J):
            send(wq.at[:, j * Gc : (j + 1) * Gc], WQX.at[d - 1, j], "wq", (d, j), xdev(d))
    T[z, tp] = tok[:, cols(z, Kz)]
    for d in range(Z):
        zs = dn(z, d, Z)
        src = T.at[zs, tp]
        if d == 0:
            src = tok.at[:, cols(z, Kz)]
        else:
            recv(src, "t1", (d,))
        for e in range(1, Y):
            send(src, T.at[zs, tp], "t2", (e, d), ydev(e))
        for f in range(1, C):
            send(src, T.at[zs, tp], "t3", (f, 0, d), cdev(f))
    for d in range(Z):
        zs = dn(z, d, Z)
        for e in range(1, Y):
            blk = T.at[zs, dn(y, e, Y) * C + c]
            recv(blk, "t2", (e, d))
            for f in range(1, C):
                send(blk, blk, "t3", (f, e, d), cdev(f))
    for d in range(Z):
        for f in range(1, C):
            for e in range(Y):
                recv(T.at[dn(z, d, Z), dn(y, e, Y) * C + dn(c, f, C)], "t3", (f, e, d))

    def tok_part(zp, xs):
        return T[zp, :, :, cols(xs, Kx)].reshape(TR, Kx)

    def dot(a, b):
        return jnp.dot(a, b, preferred_element_type=F32)

    def partial(zp, own, got):
        acc = dot(tok_part(zp, x), own)
        for d in range(1, X):
            acc = acc + dot(tok_part(zp, dn(x, d, X)), got(d))
        return acc

    for d in range(1, X):
        recv(WKX.at[d - 1], "wkv", (d, 0))
        recv(WVX.at[d - 1], "wkv", (d, 1))
    for d in list(range(1, Z)) + [0]:
        zp = up(z, d, Z)
        pk = partial(zp, wk[...], lambda q: WKX[q - 1])
        pv = partial(zp, wv[...], lambda q: WVX[q - 1])
        if d == 0:
            AKV[:, :Kc] = pk
            AKV[:, Kc:] = pv
        else:
            PKV[d - 1, :, :Kc] = pk.astype(BF16)
            PKV[d - 1, :, Kc:] = pv.astype(BF16)
            send(PKV.at[d - 1], RKV.at[d - 1], "pkv", (d,), zdev(d))

    def query_partials(j):
        for d in range(1, X):
            recv(WQX.at[d - 1, j], "wq", (d, j))
        for d in list(range(1, Z)) + [0]:
            zp = up(z, d, Z)
            pq = partial(zp, wq[:, j * Gc : (j + 1) * Gc], lambda q: WQX[q - 1, j])
            if d == 0:
                AQ[j] = pq
            else:
                PQ[j, d - 1] = pq.astype(BF16)
                send(PQ.at[j, d - 1], RQ.at[j, d - 1], "pq", (j, d), zdev(d))

    low = lax.rem(lax.broadcasted_iota(jnp.int32, (TR, hd), 1), hd // 2) < hd // 4

    def turn(raw, gain):
        v = raw.astype(BF16).astype(F32)
        v = v * lax.rsqrt(jnp.mean(v * v, axis=-1, keepdims=True) + EPS) * gain
        other = jnp.where(low, pltpu.roll(v, hd - hd // 4, 1), pltpu.roll(v, hd // 4, 1))
        return (v * cos[...] + other * sin[...]).astype(BF16)

    query_partials(0)

    for d in range(1, Z):
        recv(RKV.at[d - 1], "pkv", (d,))
    kvsum = AKV[...]
    for d in range(1, Z):
        kvsum = kvsum + RKV[d - 1].astype(F32)
    for j in range(J):
        KV[sp, :, j * hd : (j + 1) * hd] = turn(kvsum[:, j * hd : (j + 1) * hd], kg[...])
    KV[sp, :, Kc:] = kvsum[:, Kc:].astype(BF16)
    for d in range(1, Z):
        send(KV.at[sp], KV.at[sp], "kz", (d,), zdev(d))
    for e in range(1, X):
        send(KV.at[sp], KV.at[sp], "kx", (e, 0), xdev(e))

    for j in range(1, J):
        query_partials(j)
    for d in range(1, X):
        send(wo, WOX.at[d - 1], "wo", (d,), xdev(d))

    for d in range(1, Z):
        blk = KV.at[dn(z, d, Z) * X + x]
        recv(blk, "kz", (d,))
        for e in range(1, X):
            send(blk, blk, "kx", (e, d), xdev(e))
    for d in range(Z):
        for e in range(1, X):
            recv(KV.at[dn(z, d, Z) * X + dn(x, e, X)], "kx", (e, d))

    scale = hd ** (-0.5) * LOG2E
    for j in range(J):
        for d in range(1, Z):
            recv(RQ.at[j, d - 1], "pq", (j, d))

        def one_head(g, carry):
            here = cols(g, hd)
            q = AQ[j, :, here]
            for d in range(1, Z):
                q = q + RQ[j, d - 1, :, here].astype(F32)
            q = turn(q, qg[...])
            keys = KV[:, :, j * hd : (j + 1) * hd].reshape(Z * X * TR, hd)
            vals = KV[:, :, Kc + j * hd : Kc + (j + 1) * hd].reshape(Z * X * TR, hd)
            s = lax.dot_general(q, keys, (((1,), (1,)), ((), ())), preferred_element_type=F32)
            m = jnp.max(s, axis=-1, keepdims=True)
            p = jnp.exp2((s - m) * scale)
            total = jnp.sum(p, axis=-1, keepdims=True)
            o = dot(p.astype(BF16), vals)
            AT[z, j, :, here] = (o / total).astype(BF16)
            return carry

        lax.fori_loop(0, G, one_head, 0)
        for d in range(1, Z):
            send(AT.at[z, j], AT.at[z, j], "at", (j, d), zdev(d))

    for d in range(1, X):
        recv(WOX.at[d - 1], "wo", (d,))
    for d in range(Z):
        zp = dn(z, d, Z)
        if d:
            for j in range(J):
                recv(AT.at[zp, j], "at", (j, d))
        for e in range(X):
            w = wo if e == 0 else WOX.at[e - 1]
            acc = dot(AT[zp, 0], w[:Gc])
            for j in range(1, J):
                acc = acc + dot(AT[zp, j], w[j * Gc : (j + 1) * Gc])
            MB[d, :, :, :, cols(dn(x, e, X), No)] = acc.astype(BF16).reshape(Y, C, R, No)
        for f in range(1, C):
            send(MB.at[d, :, up(c, f, C)], MC.at[f - 1, d], "mc", (f, d), cdev(f))
    for d in range(Z):
        total = MB[d, :, c].astype(F32)
        for f in range(1, C):
            recv(MC.at[f - 1, d], "mc", (f, d))
            total = total + MC[f - 1, d].astype(F32)
        MS[d] = total.astype(BF16)
        for e in range(1, Y):
            send(MS.at[d, up(y, e, Y)], MY.at[e - 1, d], "my", (e, d), ydev(e))
    for d in list(range(1, Z)) + [0]:
        total = MS[d, y].astype(F32)
        for e in range(1, Y):
            recv(MY.at[e - 1, d], "my", (e, d))
            total = total + MY[e - 1, d].astype(F32)
        if d == 0:
            FB[z] = total.astype(BF16)
        else:
            FS[d - 1] = total.astype(BF16)
            send(FS.at[d - 1], FB.at[z], "ft", (d,), dev(dn(z, d, Z), x, y, c))
    for d in range(1, Z):
        recv(FB.at[up(z, d, Z)], "ft", (d,))

    square = jnp.zeros((R, 1), F32)
    for k in range(Z):
        v = FB[k].astype(F32)
        square = square + jnp.sum(v * v, axis=-1, keepdims=True)
    inv = lax.rsqrt(square * (1.0 / D) + EPS)
    for k in range(Z):
        part = slice(k * X * No, (k + 1) * X * No)
        out[:, part] = (FB[k].astype(F32) * inv * og[:, part]).astype(BF16)
    for cp in sent:
        cp.wait_send()


def split_axis(n):
    return 2 if n % 2 == 0 else 1


def fused_plan(n_sp, n_tp, tokens, q_weight, k_weight, o_weight, hd):
    X, C = split_axis(n_sp), split_axis(n_tp)
    Z, Y = n_sp // X, n_tp // C
    R, D = tokens.shape
    Kx, Qc = q_weight.shape
    Kc = k_weight.shape[1]
    J, G = Kc // hd, Qc // Kc
    Gc, TR, No = G * hd, n_tp * R, o_weight.shape[1]
    NX = X * No
    V = pltpu.VMEM
    scratch = [
        ((Z, n_tp, R, Kx * X), BF16),
        ((X - 1, J, Kx, Gc), BF16),
        ((X - 1, Kx, Kc), BF16),
        ((X - 1, Kx, Kc), BF16),
        ((X - 1, Qc, No), BF16),
        ((Z - 1, TR, 2 * Kc), BF16),
        ((Z - 1, TR, 2 * Kc), BF16),
        ((TR, 2 * Kc), F32),
        ((J, Z - 1, TR, Gc), BF16),
        ((J, Z - 1, TR, Gc), BF16),
        ((J, TR, Gc), F32),
        ((n_sp, TR, 2 * Kc), BF16),
        ((G, 16, hd), BF16),
        ((Z, J, TR, Gc), BF16),
        ((Z, Y, C, R, NX), BF16),
        ((C - 1, Z, Y, R, NX), BF16),
        ((Z, Y, R, NX), BF16),
        ((Y - 1, Z, R, NX), BF16),
        ((Z - 1, R, NX), BF16),
        ((Z, R, NX), BF16),
    ]
    size = 0
    for shape, kind in scratch:
        n = jnp.dtype(kind).itemsize
        for k in shape:
            n *= k
        size += n
    fits = min(Z, X, Y, C) > 1 and size + TR * n_sp * TR * 12 < 44 * 2**20
    return fits, (Z, X, Y, C, J, G, hd), [V(s, k) for s, k in scratch]


def fused_device(n_sp, n_tp, tokens, q_weight, k_weight, v_weight, o_weight, q_gain, k_gain, out_gain):
    hd = q_gain.shape[0]
    fits, dims, scratch = fused_plan(n_sp, n_tp, tokens, q_weight, k_weight, o_weight, hd)
    if not fits:
        return on_device(tokens, q_weight, k_weight, v_weight, o_weight, q_gain, k_gain, out_gain)
    rows = n_tp * tokens.shape[0]
    positions = lax.axis_index("sp") * rows + lax.iota(jnp.int32, rows)
    cosine, sine = tables(positions, hd)
    low = (jnp.arange(hd) % (hd // 2)) < hd // 4
    sine = jnp.where(low[None, :], -sine, sine)
    Z, X, Y, C, J = dims[:5]
    shapes = sem_shapes(Z, X, Y, C, J)
    names = list(shapes)
    for n in names:
        scratch += [pltpu.SemaphoreType.DMA(shapes[n]), pltpu.SemaphoreType.DMA(shapes[n])]
    spec = pl.BlockSpec(memory_space=pltpu.VMEM)
    return pl.pallas_call(
        functools.partial(fused_kernel, *dims, names),
        out_shape=jax.ShapeDtypeStruct(tokens.shape, BF16),
        in_specs=[spec] * 10,
        out_specs=spec,
        scratch_shapes=scratch,
        compiler_params=pltpu.CompilerParams(
            collective_id=0, has_side_effects=True, vmem_limit_bytes=60 * 2**20
        ),
    )(
        tokens, q_weight, k_weight, v_weight, o_weight,
        q_gain[None, :], k_gain[None, :], out_gain[None, :], cosine, sine,
    )


def solution(mesh):
    placed = (
        P(("sp", "tp"), None),
        P("sp", "tp"),
        P("sp", "tp"),
        P("sp", "tp"),
        P("tp", "sp"),
        P(),
        P(),
        P(),
    )
    return jax.shard_map(
        functools.partial(fused_device, mesh.shape["sp"], mesh.shape["tp"]),
        mesh=mesh, in_specs=placed, out_specs=P(("sp", "tp"), None), check_vma=False,
    )
```

```python
import functools

import jax
import jax.numpy as jnp
from jax import lax
from jax.experimental import pallas as pl
from jax.experimental.pallas import tpu as pltpu
from jax.sharding import PartitionSpec as P

GRID_W = 64


EPS = 1e-06
THETA = 10000.0


def tables(positions, head_dim):
    quarter = head_dim // 4
    grid_row = (positions // GRID_W).astype(jnp.float32)
    grid_col = (positions % GRID_W).astype(jnp.float32)
    inv_freq = 1.0 / THETA ** (jnp.arange(quarter, dtype=jnp.float32) * 2.0 / (head_dim // 2))
    ang_row = grid_row[:, None] * inv_freq[None, :]
    ang_col = grid_col[:, None] * inv_freq[None, :]
    angles = jnp.concatenate([ang_row, ang_row, ang_col, ang_col], axis=-1)
    return (jnp.cos(angles), jnp.sin(angles))


def norm_rope(raw_proj, gain_vec, positions):
    head_dim = raw_proj.shape[-1]
    values = raw_proj.astype(jnp.float32)
    values = values * lax.rsqrt(jnp.mean(values * values, axis=-1, keepdims=True) + EPS) * gain_vec
    cosine, sine_vals = tables(positions, head_dim)
    halves = values.reshape(values.shape[:-1] + (2, 2, head_dim // 4))
    rotated = jnp.stack([-halves[..., 1, :], halves[..., 0, :]], axis=-2).reshape(values.shape)
    return values * cosine[:, None, :] + rotated * sine_vals[:, None, :]


def on_device(tokens, q_weight, k_weight, v_weight, o_weight, q_gain, k_gain, out_gain):
    q_full, k_full, v_full, o_full = (
        lax.all_gather(q_weight, "sp", axis=0, tiled=True),
        lax.all_gather(k_weight, "sp", axis=0, tiled=True),
        lax.all_gather(v_weight, "sp", axis=0, tiled=True),
        lax.all_gather(o_weight, "sp", axis=1, tiled=True),
    )
    query_cols = q_full.shape[1]
    value_cols = k_full.shape[1]
    head_dim = q_gain.shape[0]
    local_kv = value_cols // head_dim
    groups = query_cols // value_cols

    def project(portion):
        return jnp.concatenate(
            [
                jnp.dot(portion, q_full, preferred_element_type=jnp.float32),
                jnp.dot(portion, k_full, preferred_element_type=jnp.float32),
                jnp.dot(portion, v_full, preferred_element_type=jnp.float32),
            ],
            axis=1,
        )

    projected = project(lax.all_gather(tokens, "tp", axis=0, tiled=True)).astype(jnp.bfloat16)
    tok_rows = projected.shape[0]
    positions = lax.axis_index("sp") * tok_rows + lax.iota(jnp.int32, tok_rows)
    queries = norm_rope(
        projected[:, :query_cols].reshape(tok_rows, local_kv * groups, head_dim), q_gain, positions
    )
    queries = queries.astype(jnp.bfloat16).reshape(tok_rows, local_kv, groups, head_dim)
    keys = norm_rope(
        projected[:, query_cols : query_cols + value_cols].reshape(tok_rows, local_kv, head_dim),
        k_gain,
        positions,
    )
    keys = keys.astype(jnp.bfloat16)
    values = projected[:, query_cols + value_cols :].reshape(tok_rows, local_kv, head_dim)
    score_scale = head_dim ** (-0.5)

    def absorb(state_in, key_blk, val_blk):
        run_max, run_sum, run_acc = state_in
        scores = (
            jnp.einsum("qkgd,tkd->kgqt", queries, key_blk, preferred_element_type=jnp.float32)
            * score_scale
        )
        new_max = jnp.maximum(run_max, jnp.max(scores, axis=-1))
        shrink = jnp.exp(run_max - new_max)
        probs_blk = jnp.exp(scores - new_max[..., None])
        run_sum = run_sum * shrink + jnp.sum(probs_blk, axis=-1)
        update = jnp.einsum(
            "kgqt,tkd->kgqd",
            probs_blk.astype(jnp.bfloat16),
            val_blk,
            preferred_element_type=jnp.float32,
        )
        run_acc = run_acc * shrink[..., None] + update
        return (new_max, run_sum, run_acc)

    def fold_keys(state_in, pieces):
        key_piece, val_piece = pieces
        row_count = key_piece.shape[0]
        width = 512 if row_count % 512 == 0 else row_count
        key_blocks = key_piece.reshape(row_count // width, width, local_kv, head_dim)
        val_blocks = val_piece.reshape(row_count // width, width, local_kv, head_dim)

        def scan_step(state_now, block_pair):
            return (absorb(state_now, block_pair[0], block_pair[1]), None)

        state_out, unused = lax.scan(scan_step, state_in, (key_blocks, val_blocks))
        return state_out

    initial = (
        jnp.full((local_kv, groups, tok_rows), -1e30, jnp.float32),
        jnp.zeros((local_kv, groups, tok_rows), jnp.float32),
        jnp.zeros((local_kv, groups, tok_rows, head_dim), jnp.float32),
    )
    run_max, run_sum, run_acc = fold_keys(
        initial,
        (
            lax.all_gather(keys, "sp", axis=0, tiled=True),
            lax.all_gather(values, "sp", axis=0, tiled=True),
        ),
    )
    attended = (
        (run_acc / run_sum[..., None])
        .transpose(2, 0, 1, 3)
        .reshape(tok_rows, query_cols)
        .astype(jnp.bfloat16)
    )

    def out_term():
        picked = lax.slice_in_dim(attended, 0, own_rows * lax.axis_size("tp"), axis=0)
        return jnp.dot(picked, o_full, preferred_element_type=jnp.float32)

    own_rows = tokens.shape[0]
    mixed = lax.psum_scatter(
        out_term().astype(jnp.bfloat16), "tp", scatter_dimension=0, tiled=True
    ).astype(jnp.float32)
    normed = mixed * lax.rsqrt(jnp.mean(mixed * mixed, axis=-1, keepdims=True) + EPS) * out_gain
    return normed.astype(jnp.bfloat16)


MESH = pl.DeviceIdType.MESH
F32, BF16 = jnp.float32, jnp.bfloat16
LOG2E = 1.4426950408889634


def sem_shapes(Z, X, Y, C, J):
    return {
        "t1": (Z,),
        "t2": (Y, Z),
        "t3": (C, Y, Z),
        "wkv": (X, 2),
        "wq": (X, J),
        "wo": (X,),
        "pkv": (Z + 1,),
        "pq": (J, Z + 1),
        "kz": (Z + 1,),
        "kx": (X, Z),
        "at": (J, Z + 1),
        "mc": (C, Z),
        "my": (Y, Z),
        "ft": (Z,),
    }


def fused_kernel(Z, X, Y, C, J, G, hd, names, *refs):
    (tok, wq, wk, wv, wo, qg, kg, og, cos, sin, out) = refs[:11]
    (T, WQX, WKX, WVX, WOX, PKV, RKV, AKV, PQ, RQ, AQ, KV, AT, MB, MC, MS, MY, FS, FB) = refs[11:30]
    sems = {n: (refs[30 + 2 * i], refs[31 + 2 * i]) for i, n in enumerate(names)}

    sp, tp = lax.axis_index("sp"), lax.axis_index("tp")
    z, x = lax.div(sp, X), lax.rem(sp, X)
    y, c = lax.div(tp, C), lax.rem(tp, C)
    R, D = tok.shape
    TP = Y * C
    TR = TP * R
    Kx = wq.shape[0]
    Kz = Kx * X
    Gc = G * hd
    Kc = J * hd
    No = wo.shape[1]

    def up(v, d, n):
        return lax.rem(v + d, n)

    def dn(v, d, n):
        return lax.rem(v + n - d, n)

    def dev(zz, xx, yy, cc):
        return {"sp": zz * X + xx, "tp": yy * C + cc}

    def zdev(d):
        return dev(up(z, d, Z), x, y, c)

    def xdev(d):
        return dev(z, up(x, d, X), y, c)

    def ydev(d):
        return dev(z, x, up(y, d, Y), c)

    def cdev(d):
        return dev(z, x, y, up(c, d, C))

    sent = []

    def send(src, dst, name, idx, to, ridx=None, when=None):
        s, r = sems[name]
        ridx = idx if ridx is None else ridx

        def make():
            return pltpu.make_async_remote_copy(
                src_ref=src, dst_ref=dst, send_sem=s.at[idx], recv_sem=r.at[ridx],
                device_id=to, device_id_type=MESH,
            )

        if when is None:
            make().start()
        else:
            pl.when(when)(lambda: make().start())
        sent.append((make, when))

    def recv(dst, name, idx):
        s, r = sems[name]
        pltpu.make_async_remote_copy(
            src_ref=dst, dst_ref=dst, send_sem=s.at[idx], recv_sem=r.at[idx],
            device_id=cdev(1), device_id_type=MESH,
        ).wait_recv()

    def cols(k, n):
        return pl.ds(pl.multiple_of(k * n, n), n)

    def pick(rows_by_z, n):
        v = 0
        for k in range(Z):
            v = v + jnp.where(z == k, rows_by_z[k][n], 0)
        return v

    near = [sorted([k for k in range(Z) if k != q], key=lambda k: abs(k - q)) for q in range(Z)]
    far = [sorted(r, key=lambda k: -abs(k - q)) for q, r in enumerate(near)]
    above, below = z < Z - 1, z > 0

    def line_own(ref, at, name, pre):
        send(ref.at[at], ref.at[at], name, pre + (z,), dev(z + 1, x, y, c), when=above)
        send(ref.at[at], ref.at[at], name, pre + (Z,), dev(z - 1, x, y, c), ridx=pre + (z,), when=below)

    def line_hop(zp, ref, at, name, pre):
        recv(ref.at[at], name, pre + (zp,))
        go_up = jnp.logical_and(zp < z, above)
        go_down = jnp.logical_and(zp > z, below)
        step = jnp.where(zp < z, 1, -1)
        send(ref.at[at], ref.at[at], name, pre + (zp,), dev(z + step, x, y, c), when=jnp.logical_or(go_up, go_down))

    barrier = pltpu.get_barrier_semaphore()
    peers = [zdev(d) for d in range(1, Z)] + [xdev(d) for d in range(1, X)]
    peers += [ydev(d) for d in range(1, Y)] + [cdev(d) for d in range(1, C)]
    for p in peers:
        pl.semaphore_signal(barrier, inc=1, device_id=p, device_id_type=MESH)
    pl.semaphore_wait(barrier, len(peers))

    for d in range(1, Z):
        send(tok.at[:, cols(up(z, d, Z), Kz)], T.at[z, tp], "t1", (d,), zdev(d))
    for d in range(1, X):
        send(wk, WKX.at[d - 1], "wkv", (d, 0), xdev(d))
        send(wv, WVX.at[d - 1], "wkv", (d, 1), xdev(d))
        for j in range(J):
            send(wq.at[:, j * Gc : (j + 1) * Gc], WQX.at[d - 1, j], "wq", (d, j), xdev(d))
    T[z, tp] = tok[:, cols(z, Kz)]
    for d in range(Z):
        zs = dn(z, d, Z)
        src = T.at[zs, tp]
        if d == 0:
            src = tok.at[:, cols(z, Kz)]
        else:
            recv(src, "t1", (d,))
        for e in range(1, Y):
            send(src, T.at[zs, tp], "t2", (e, d), ydev(e))
        for f in range(1, C):
            send(src, T.at[zs, tp], "t3", (f, 0, d), cdev(f))
    for d in range(Z):
        zs = dn(z, d, Z)
        for e in range(1, Y):
            blk = T.at[zs, dn(y, e, Y) * C + c]
            recv(blk, "t2", (e, d))
            for f in range(1, C):
                send(blk, blk, "t3", (f, e, d), cdev(f))
    for d in range(Z):
        for f in range(1, C):
            for e in range(Y):
                recv(T.at[dn(z, d, Z), dn(y, e, Y) * C + dn(c, f, C)], "t3", (f, e, d))

    def tok_part(zp, xs):
        return T[zp, :, :, cols(xs, Kx)].reshape(TR, Kx)

    def dot(a, b):
        return jnp.dot(a, b, preferred_element_type=F32)

    def partial(zp, own, got):
        acc = dot(tok_part(zp, x), own)
        for d in range(1, X):
            acc = acc + dot(tok_part(zp, dn(x, d, X)), got(d))
        return acc

    def line_sum(n, acc_of, pre, Ps, Rs, name):
        zp = pick(far, n)
        acc = acc_of(zp)
        relay = jnp.where(zp > z, z, Z - 1 - z) > 0

        @pl.when(relay)
        def _():
            recv(Rs(zp), name, pre + (zp,))
            Ps(n)[...] = (acc + Rs(zp)[...].astype(F32)).astype(BF16)

        @pl.when(jnp.logical_not(relay))
        def _():
            Ps(n)[...] = acc.astype(BF16)

        step = jnp.where(zp > z, 1, -1)
        slot = jnp.where(zp == z - 1, Z, zp)
        send(Ps(n), Rs(slot), name, pre + (n,), dev(z + step, x, y, c), ridx=pre + (slot,))

    def line_total(A, pre, Rs, name):
        for cond, slot in ((below, z), (above, Z)):

            @pl.when(cond)
            def _():
                recv(Rs(slot), name, pre + (slot,))
                A[...] = A[...] + Rs(slot)[...].astype(F32)

    def kv_partial(zp):
        pk = partial(zp, wk[...], lambda q: WKX[q - 1])
        pv = partial(zp, wv[...], lambda q: WVX[q - 1])
        return jnp.concatenate([pk, pv], axis=1)

    def kv_step(n):
        line_sum(n, kv_partial, (), lambda k: PKV.at[k], lambda k: RKV.at[k], "pkv")

    def q_partial(j):
        return lambda zp: partial(zp, wq[:, j * Gc : (j + 1) * Gc], lambda q: WQX[q - 1, j])

    def q_step(j, n):
        if n == 0:
            for d in range(1, X):
                recv(WQX.at[d - 1, j], "wq", (d, j))
        line_sum(n, q_partial(j), (j,), lambda k: PQ.at[j, k], lambda k: RQ.at[j, k], "pq")
        if n == Z - 2:
            AQ[j] = q_partial(j)(z)

    for d in range(1, X):
        recv(WKX.at[d - 1], "wkv", (d, 0))
        recv(WVX.at[d - 1], "wkv", (d, 1))
    for n in range(Z - 1):
        kv_step(n)
    AKV[...] = kv_partial(z)
    q_steps = [(j, n) for j in range(J) for n in range(Z - 1)]
    q_step(*q_steps.pop(0))

    low = lax.rem(lax.broadcasted_iota(jnp.int32, (TR, hd), 1), hd // 2) < hd // 4

    def turn(raw, gain):
        v = raw.astype(BF16).astype(F32)
        v = v * lax.rsqrt(jnp.mean(v * v, axis=-1, keepdims=True) + EPS) * gain
        other = jnp.where(low, pltpu.roll(v, hd - hd // 4, 1), pltpu.roll(v, hd // 4, 1))
        return (v * cos[...] + other * sin[...]).astype(BF16)

    line_total(AKV, (), lambda k: RKV.at[k], "pkv")
    for j in range(J):
        KV[sp, :, j * hd : (j + 1) * hd] = turn(AKV[:, j * hd : (j + 1) * hd], kg[...])
    KV[sp, :, Kc:] = AKV[:, Kc:].astype(BF16)
    line_own(KV, sp, "kz", ())
    for e in range(1, X):
        send(KV.at[sp], KV.at[sp], "kx", (e, z), xdev(e))

    def kv_hop(n):
        zp = pick(near, n)
        line_hop(zp, KV, zp * X + x, "kz", ())
        for e in range(1, X):
            send(KV.at[zp * X + x], KV.at[zp * X + x], "kx", (e, zp), xdev(e))

    for n in range(Z - 1):
        if q_steps:
            q_step(*q_steps.pop(0))
        kv_hop(n)
    for step in q_steps:
        q_step(*step)
    for d in range(1, X):
        send(wo, WOX.at[d - 1], "wo", (d,), xdev(d))
    for k in range(Z):
        for e in range(1, X):
            recv(KV.at[k * X + dn(x, e, X)], "kx", (e, k))

    scale = hd ** (-0.5) * LOG2E
    for j in range(J):
        line_total(AQ.at[j], (j,), lambda k: RQ.at[j, k], "pq")

        def one_head(g, carry):
            here = cols(g, hd)
            q = turn(AQ[j, :, here], qg[...])
            keys = KV[:, :, j * hd : (j + 1) * hd].reshape(Z * X * TR, hd)
            vals = KV[:, :, Kc + j * hd : Kc + (j + 1) * hd].reshape(Z * X * TR, hd)
            s = lax.dot_general(q, keys, (((1,), (1,)), ((), ())), preferred_element_type=F32)
            m = jnp.max(s, axis=-1, keepdims=True)
            p = jnp.exp2((s - m) * scale)
            total = jnp.sum(p, axis=-1, keepdims=True)
            o = dot(p.astype(BF16), vals)
            AT[z, j, :, here] = (o / total).astype(BF16)
            return carry

        lax.fori_loop(0, G, one_head, 0)
        for up_down in ((z, z + 1, above), (Z, z - 1, below)):
            send(AT.at[z, j], AT.at[z, j], "at", (j, up_down[0]), dev(up_down[1], x, y, c), ridx=(j, z), when=up_down[2])

    for d in range(1, X):
        recv(WOX.at[d - 1], "wo", (d,))

    def out_block(zp):
        for e in range(X):
            w = wo if e == 0 else WOX.at[e - 1]
            acc = dot(AT[zp, 0], w[:Gc])
            for j in range(1, J):
                acc = acc + dot(AT[zp, j], w[j * Gc : (j + 1) * Gc])
            MB[zp, :, :, :, cols(dn(x, e, X), No)] = acc.astype(BF16).reshape(Y, C, R, No)
        for f in range(1, C):
            send(MB.at[zp, :, up(c, f, C)], MC.at[f - 1, zp], "mc", (f, zp), cdev(f))

    def core_block(zp):
        total = MB[zp, :, c].astype(F32)
        for f in range(1, C):
            recv(MC.at[f - 1, zp], "mc", (f, zp))
            total = total + MC[f - 1, zp].astype(F32)
        MS[zp] = total.astype(BF16)
        for e in range(1, Y):
            send(MS.at[zp, up(y, e, Y)], MY.at[e - 1, zp], "my", (e, zp), ydev(e))

    def row_block(zp, n):
        total = MS[zp, y].astype(F32)
        for e in range(1, Y):
            recv(MY.at[e - 1, zp], "my", (e, zp))
            total = total + MY[e - 1, zp].astype(F32)
        if n == 0:
            FB[z] = total.astype(BF16)
        else:
            FS[n - 1] = total.astype(BF16)
            send(FS.at[n - 1], FB.at[z], "ft", (n,), dev(zp, x, y, c), ridx=(z,))

    blocks = [z] + [pick(near, n) for n in range(Z - 1)]
    for n in range(Z + 2):
        if n < Z:
            zp = blocks[n]
            if n:
                for j in range(J):
                    blk = AT.at[zp, j]
                    recv(blk, "at", (j, zp))
                    onward = jnp.where(zp < z, Z - 1 - z, z) > 0
                    step = jnp.where(zp < z, 1, -1)
                    send(blk, blk, "at", (j, zp), dev(z + step, x, y, c), when=onward)
            out_block(zp)
        if 1 <= n <= Z:
            core_block(blocks[n - 1])
        if n >= 2:
            row_block(blocks[n - 2], n - 2)
    for n in range(1, Z):
        recv(FB.at[blocks[n]], "ft", (blocks[n],))

    square = jnp.zeros((R, 1), F32)
    for k in range(Z):
        v = FB[k].astype(F32)
        square = square + jnp.sum(v * v, axis=-1, keepdims=True)
    inv = lax.rsqrt(square * (1.0 / D) + EPS)
    for k in range(Z):
        part = slice(k * X * No, (k + 1) * X * No)
        out[:, part] = (FB[k].astype(F32) * inv * og[:, part]).astype(BF16)
    for make, when in sent:
        if when is None:
            make().wait_send()
        else:
            pl.when(when)(lambda make=make: make().wait_send())


def split_axis(n):
    return 2 if n % 2 == 0 else 1


def fused_plan(n_sp, n_tp, tokens, q_weight, k_weight, o_weight, hd):
    X, C = split_axis(n_sp), split_axis(n_tp)
    Z, Y = n_sp // X, n_tp // C
    R, D = tokens.shape
    Kx, Qc = q_weight.shape
    Kc = k_weight.shape[1]
    J, G = Kc // hd, Qc // Kc
    Gc, TR, No = G * hd, n_tp * R, o_weight.shape[1]
    NX = X * No
    V = pltpu.VMEM
    scratch = [
        ((Z, n_tp, R, Kx * X), BF16),
        ((X - 1, J, Kx, Gc), BF16),
        ((X - 1, Kx, Kc), BF16),
        ((X - 1, Kx, Kc), BF16),
        ((X - 1, Qc, No), BF16),
        ((Z - 1, TR, 2 * Kc), BF16),
        ((Z + 1, TR, 2 * Kc), BF16),
        ((TR, 2 * Kc), F32),
        ((J, Z - 1, TR, Gc), BF16),
        ((J, Z + 1, TR, Gc), BF16),
        ((J, TR, Gc), F32),
        ((n_sp, TR, 2 * Kc), BF16),
        ((Z, J, TR, Gc), BF16),
        ((Z, Y, C, R, NX), BF16),
        ((C - 1, Z, Y, R, NX), BF16),
        ((Z, Y, R, NX), BF16),
        ((Y - 1, Z, R, NX), BF16),
        ((Z - 1, R, NX), BF16),
        ((Z, R, NX), BF16),
    ]
    size = 0
    for shape, kind in scratch:
        n = jnp.dtype(kind).itemsize
        for k in shape:
            n *= k
        size += n
    fits = min(Z, X, Y, C) > 1 and size + TR * n_sp * TR * 12 < 44 * 2**20
    return fits, (Z, X, Y, C, J, G, hd), [V(s, k) for s, k in scratch]


def fused_device(n_sp, n_tp, tokens, q_weight, k_weight, v_weight, o_weight, q_gain, k_gain, out_gain):
    hd = q_gain.shape[0]
    fits, dims, scratch = fused_plan(n_sp, n_tp, tokens, q_weight, k_weight, o_weight, hd)
    if not fits:
        return on_device(tokens, q_weight, k_weight, v_weight, o_weight, q_gain, k_gain, out_gain)
    rows = n_tp * tokens.shape[0]
    positions = lax.axis_index("sp") * rows + lax.iota(jnp.int32, rows)
    cosine, sine = tables(positions, hd)
    low = (jnp.arange(hd) % (hd // 2)) < hd // 4
    sine = jnp.where(low[None, :], -sine, sine)
    Z, X, Y, C, J = dims[:5]
    shapes = sem_shapes(Z, X, Y, C, J)
    names = list(shapes)
    for n in names:
        scratch += [pltpu.SemaphoreType.DMA(shapes[n]), pltpu.SemaphoreType.DMA(shapes[n])]
    spec = pl.BlockSpec(memory_space=pltpu.VMEM)
    return pl.pallas_call(
        functools.partial(fused_kernel, *dims, names),
        out_shape=jax.ShapeDtypeStruct(tokens.shape, BF16),
        in_specs=[spec] * 10,
        out_specs=spec,
        scratch_shapes=scratch,
        compiler_params=pltpu.CompilerParams(
            collective_id=0, has_side_effects=True, vmem_limit_bytes=60 * 2**20
        ),
    )(
        tokens, q_weight, k_weight, v_weight, o_weight,
        q_gain[None, :], k_gain[None, :], out_gain[None, :], cosine, sine,
    )


def solution(mesh):
    placed = (
        P(("sp", "tp"), None),
        P("sp", "tp"),
        P("sp", "tp"),
        P("sp", "tp"),
        P("tp", "sp"),
        P(),
        P(),
        P(),
    )
    return jax.shard_map(
        functools.partial(fused_device, mesh.shape["sp"], mesh.shape["tp"]),
        mesh=mesh, in_specs=placed, out_specs=P(("sp", "tp"), None), check_vma=False,
    )
```

```python
import functools

import jax
import jax.numpy as jnp
from jax import lax
from jax.experimental import pallas as pl
from jax.experimental.pallas import tpu as pltpu
from jax.sharding import PartitionSpec as P

GRID_W = 64


EPS = 1e-06
THETA = 10000.0


def tables(positions, head_dim):
    quarter = head_dim // 4
    grid_row = (positions // GRID_W).astype(jnp.float32)
    grid_col = (positions % GRID_W).astype(jnp.float32)
    inv_freq = 1.0 / THETA ** (jnp.arange(quarter, dtype=jnp.float32) * 2.0 / (head_dim // 2))
    ang_row = grid_row[:, None] * inv_freq[None, :]
    ang_col = grid_col[:, None] * inv_freq[None, :]
    angles = jnp.concatenate([ang_row, ang_row, ang_col, ang_col], axis=-1)
    return (jnp.cos(angles), jnp.sin(angles))


def norm_rope(raw_proj, gain_vec, positions):
    head_dim = raw_proj.shape[-1]
    values = raw_proj.astype(jnp.float32)
    values = values * lax.rsqrt(jnp.mean(values * values, axis=-1, keepdims=True) + EPS) * gain_vec
    cosine, sine_vals = tables(positions, head_dim)
    halves = values.reshape(values.shape[:-1] + (2, 2, head_dim // 4))
    rotated = jnp.stack([-halves[..., 1, :], halves[..., 0, :]], axis=-2).reshape(values.shape)
    return values * cosine[:, None, :] + rotated * sine_vals[:, None, :]


def on_device(tokens, q_weight, k_weight, v_weight, o_weight, q_gain, k_gain, out_gain):
    q_full, k_full, v_full, o_full = (
        lax.all_gather(q_weight, "sp", axis=0, tiled=True),
        lax.all_gather(k_weight, "sp", axis=0, tiled=True),
        lax.all_gather(v_weight, "sp", axis=0, tiled=True),
        lax.all_gather(o_weight, "sp", axis=1, tiled=True),
    )
    query_cols = q_full.shape[1]
    value_cols = k_full.shape[1]
    head_dim = q_gain.shape[0]
    local_kv = value_cols // head_dim
    groups = query_cols // value_cols

    def project(portion):
        return jnp.concatenate(
            [
                jnp.dot(portion, q_full, preferred_element_type=jnp.float32),
                jnp.dot(portion, k_full, preferred_element_type=jnp.float32),
                jnp.dot(portion, v_full, preferred_element_type=jnp.float32),
            ],
            axis=1,
        )

    projected = project(lax.all_gather(tokens, "tp", axis=0, tiled=True)).astype(jnp.bfloat16)
    tok_rows = projected.shape[0]
    positions = lax.axis_index("sp") * tok_rows + lax.iota(jnp.int32, tok_rows)
    queries = norm_rope(
        projected[:, :query_cols].reshape(tok_rows, local_kv * groups, head_dim), q_gain, positions
    )
    queries = queries.astype(jnp.bfloat16).reshape(tok_rows, local_kv, groups, head_dim)
    keys = norm_rope(
        projected[:, query_cols : query_cols + value_cols].reshape(tok_rows, local_kv, head_dim),
        k_gain,
        positions,
    )
    keys = keys.astype(jnp.bfloat16)
    values = projected[:, query_cols + value_cols :].reshape(tok_rows, local_kv, head_dim)
    score_scale = head_dim ** (-0.5)

    def absorb(state_in, key_blk, val_blk):
        run_max, run_sum, run_acc = state_in
        scores = (
            jnp.einsum("qkgd,tkd->kgqt", queries, key_blk, preferred_element_type=jnp.float32)
            * score_scale
        )
        new_max = jnp.maximum(run_max, jnp.max(scores, axis=-1))
        shrink = jnp.exp(run_max - new_max)
        probs_blk = jnp.exp(scores - new_max[..., None])
        run_sum = run_sum * shrink + jnp.sum(probs_blk, axis=-1)
        update = jnp.einsum(
            "kgqt,tkd->kgqd",
            probs_blk.astype(jnp.bfloat16),
            val_blk,
            preferred_element_type=jnp.float32,
        )
        run_acc = run_acc * shrink[..., None] + update
        return (new_max, run_sum, run_acc)

    def fold_keys(state_in, pieces):
        key_piece, val_piece = pieces
        row_count = key_piece.shape[0]
        width = 512 if row_count % 512 == 0 else row_count
        key_blocks = key_piece.reshape(row_count // width, width, local_kv, head_dim)
        val_blocks = val_piece.reshape(row_count // width, width, local_kv, head_dim)

        def scan_step(state_now, block_pair):
            return (absorb(state_now, block_pair[0], block_pair[1]), None)

        state_out, unused = lax.scan(scan_step, state_in, (key_blocks, val_blocks))
        return state_out

    initial = (
        jnp.full((local_kv, groups, tok_rows), -1e30, jnp.float32),
        jnp.zeros((local_kv, groups, tok_rows), jnp.float32),
        jnp.zeros((local_kv, groups, tok_rows, head_dim), jnp.float32),
    )
    run_max, run_sum, run_acc = fold_keys(
        initial,
        (
            lax.all_gather(keys, "sp", axis=0, tiled=True),
            lax.all_gather(values, "sp", axis=0, tiled=True),
        ),
    )
    attended = (
        (run_acc / run_sum[..., None])
        .transpose(2, 0, 1, 3)
        .reshape(tok_rows, query_cols)
        .astype(jnp.bfloat16)
    )

    def out_term():
        picked = lax.slice_in_dim(attended, 0, own_rows * lax.axis_size("tp"), axis=0)
        return jnp.dot(picked, o_full, preferred_element_type=jnp.float32)

    own_rows = tokens.shape[0]
    mixed = lax.psum_scatter(
        out_term().astype(jnp.bfloat16), "tp", scatter_dimension=0, tiled=True
    ).astype(jnp.float32)
    normed = mixed * lax.rsqrt(jnp.mean(mixed * mixed, axis=-1, keepdims=True) + EPS) * out_gain
    return normed.astype(jnp.bfloat16)


MESH = pl.DeviceIdType.MESH
F32, BF16 = jnp.float32, jnp.bfloat16
LOG2E = 1.4426950408889634
H = 2


def sem_shapes(Z, X, Y, C, J):
    return {
        "t1": (Z,),
        "t2": (Y, Z),
        "t3": (C, Y, Z),
        "wkv": (X, 2),
        "wq": (X, J),
        "wo": (X, J),
        "pkv": (Z + 1, H),
        "pq": (J, Z + 1, H),
        "kz": (Z + 1,),
        "kx": (X, Z),
        "at": (J, Z + 1),
        "mc": (C, Z),
        "my": (Y, Z),
        "ft": (Z,),
    }


def fused_kernel(Z, X, Y, C, J, G, hd, names, *refs):
    (tok, wq, wk, wv, wo, qg, kg, og, cos, sin, out) = refs[:11]
    (T, WQX, WKX, WVX, WOX, PKV, RKV, AKV, PQ, RQ, AQ, KV, AT, MB, MC, MS, MY, FS, FB) = refs[11:30]
    sems = {n: (refs[30 + 2 * i], refs[31 + 2 * i]) for i, n in enumerate(names)}

    sp, tp = lax.axis_index("sp"), lax.axis_index("tp")
    z, x = lax.div(sp, X), lax.rem(sp, X)
    y, c = lax.div(tp, C), lax.rem(tp, C)
    R, D = tok.shape
    TP = Y * C
    TR = TP * R
    Kx = wq.shape[0]
    Kz = Kx * X
    Gc = G * hd
    Kc = J * hd
    No = wo.shape[1]

    def up(v, d, n):
        return lax.rem(v + d, n)

    def dn(v, d, n):
        return lax.rem(v + n - d, n)

    def dev(zz, xx, yy, cc):
        return {"sp": zz * X + xx, "tp": yy * C + cc}

    def zdev(d):
        return dev(up(z, d, Z), x, y, c)

    def xdev(d):
        return dev(z, up(x, d, X), y, c)

    def ydev(d):
        return dev(z, x, up(y, d, Y), c)

    def cdev(d):
        return dev(z, x, y, up(c, d, C))

    sent = []

    def wait_for(src, name, idx):
        return lambda: pltpu.make_async_remote_copy(
            src_ref=src, dst_ref=src, send_sem=sems[name][0].at[idx], recv_sem=sems[name][1].at[idx],
            device_id=cdev(1), device_id_type=MESH,
        ).wait_send()

    def send(src, dst, name, idx, to, ridx=None, when=None, keep=True):
        s, r = sems[name]
        ridx = idx if ridx is None else ridx

        def make():
            return pltpu.make_async_remote_copy(
                src_ref=src, dst_ref=dst, send_sem=s.at[idx], recv_sem=r.at[ridx],
                device_id=to, device_id_type=MESH,
            )

        if when is None:
            make().start()
        else:
            pl.when(when)(lambda: make().start())
        if keep:
            sent.append((wait_for(src, name, idx), when))

    def recv(dst, name, idx):
        s, r = sems[name]
        pltpu.make_async_remote_copy(
            src_ref=dst, dst_ref=dst, send_sem=s.at[idx], recv_sem=r.at[idx],
            device_id=cdev(1), device_id_type=MESH,
        ).wait_recv()

    def cols(k, n):
        return pl.ds(pl.multiple_of(k * n, n), n)

    def pick(rows_by_z, n):
        v = 0
        for k in range(Z):
            v = v + jnp.where(z == k, rows_by_z[k][n], 0)
        return v

    near = [sorted([k for k in range(Z) if k != q], key=lambda k: abs(k - q)) for q in range(Z)]
    far = [sorted(r, key=lambda k: -abs(k - q)) for q, r in enumerate(near)]
    above, below = z < Z - 1, z > 0

    def line_own(ref, at, name, pre):
        send(ref.at[at], ref.at[at], name, pre + (z,), dev(z + 1, x, y, c), when=above)
        send(ref.at[at], ref.at[at], name, pre + (Z,), dev(z - 1, x, y, c), ridx=pre + (z,), when=below)

    def line_hop(zp, ref, at, name, pre):
        recv(ref.at[at], name, pre + (zp,))
        go_up = jnp.logical_and(zp < z, above)
        go_down = jnp.logical_and(zp > z, below)
        step = jnp.where(zp < z, 1, -1)
        send(ref.at[at], ref.at[at], name, pre + (zp,), dev(z + step, x, y, c), when=jnp.logical_or(go_up, go_down))

    barrier = pltpu.get_barrier_semaphore()
    peers = [zdev(d) for d in range(1, Z)] + [xdev(d) for d in range(1, X)]
    peers += [ydev(d) for d in range(1, Y)] + [cdev(d) for d in range(1, C)]
    for p in peers:
        pl.semaphore_signal(barrier, inc=1, device_id=p, device_id_type=MESH)
    pl.semaphore_wait(barrier, len(peers))

    for d in range(1, Z):
        send(tok.at[:, cols(up(z, d, Z), Kz)], T.at[z, tp], "t1", (d,), zdev(d))
    for d in range(1, X):
        send(wk, WKX.at[d - 1], "wkv", (d, 0), xdev(d))
        send(wv, WVX.at[d - 1], "wkv", (d, 1), xdev(d))
        for j in range(J):
            send(wq.at[:, j * Gc : (j + 1) * Gc], WQX.at[d - 1, j], "wq", (d, j), xdev(d))
    T[z, tp] = tok[:, cols(z, Kz)]
    for d in range(Z):
        zs = dn(z, d, Z)
        src = T.at[zs, tp]
        if d == 0:
            src = tok.at[:, cols(z, Kz)]
        else:
            recv(src, "t1", (d,))
        for e in range(1, Y):
            send(src, T.at[zs, tp], "t2", (e, d), ydev(e))
        for f in range(1, C):
            send(src, T.at[zs, tp], "t3", (f, 0, d), cdev(f))
    for d in range(Z):
        zs = dn(z, d, Z)
        for e in range(1, Y):
            blk = T.at[zs, dn(y, e, Y) * C + c]
            recv(blk, "t2", (e, d))
            for f in range(1, C):
                send(blk, blk, "t3", (f, e, d), cdev(f))
    for d in range(Z):
        for f in range(1, C):
            for e in range(Y):
                recv(T.at[dn(z, d, Z), dn(y, e, Y) * C + dn(c, f, C)], "t3", (f, e, d))

    def tok_part(zp, xs):
        return T[zp, :, :, cols(xs, Kx)].reshape(TR, Kx)

    def dot(a, b):
        return jnp.dot(a, b, preferred_element_type=F32)

    def partial(zp, own, got):
        acc = dot(tok_part(zp, x), own)
        for d in range(1, X):
            acc = acc + dot(tok_part(zp, dn(x, d, X)), got(d))
        return acc

    def line_sum(n, acc_of, pre, Ps, Rs, name):
        zp = pick(far, n)
        acc = acc_of(zp)
        relay = jnp.where(zp > z, z, Z - 1 - z) > 0

        step = jnp.where(zp > z, 1, -1)
        slot = jnp.where(zp == z - 1, Z, zp)
        for h in range(H):
            rows = slice(h * TR // H, (h + 1) * TR // H)
            part = acc[rows]

            @pl.when(relay)
            def _():
                got = Rs(zp).at[rows]
                recv(got, name, pre + (zp, h))
                Ps(n)[rows] = (part + got[...].astype(F32)).astype(BF16)

            @pl.when(jnp.logical_not(relay))
            def _():
                Ps(n)[rows] = part.astype(BF16)

            send(
                Ps(n).at[rows], Rs(slot).at[rows], name, pre + (n, h),
                dev(z + step, x, y, c), ridx=pre + (slot, h), keep=False,
            )

    def line_total(A, pre, Rs, name):
        for cond, slot in ((below, z), (above, Z)):

            @pl.when(cond)
            def _():
                for h in range(H):
                    recv(Rs(slot).at[h * TR // H : (h + 1) * TR // H], name, pre + (slot, h))
                A[...] = A[...] + Rs(slot)[...].astype(F32)

    def kv_partial(zp):
        pk = partial(zp, wk[...], lambda q: WKX[q - 1])
        pv = partial(zp, wv[...], lambda q: WVX[q - 1])
        return jnp.concatenate([pk, pv], axis=1)

    def kv_step(n):
        line_sum(n, kv_partial, (), lambda k: PKV.at[k], lambda k: RKV.at[k], "pkv")

    def q_partial(j):
        return lambda zp: partial(zp, wq[:, j * Gc : (j + 1) * Gc], lambda q: WQX[q - 1, j])

    def q_step(j, n):
        if n == 0:
            for d in range(1, X):
                recv(WQX.at[d - 1, j], "wq", (d, j))
        line_sum(n, q_partial(j), (j,), lambda k: PQ.at[j, k], lambda k: RQ.at[j, k], "pq")
        if n == Z - 2:
            AQ[j] = q_partial(j)(z)

    for d in range(1, X):
        recv(WKX.at[d - 1], "wkv", (d, 0))
        recv(WVX.at[d - 1], "wkv", (d, 1))
    for n in range(Z - 1):
        kv_step(n)
    AKV[...] = kv_partial(z)
    q_steps = [(j, n) for j in range(J) for n in range(Z - 1)]
    q_step(*q_steps.pop(0))
    def out_weight(j):
        rows = slice(j * Gc, (j + 1) * Gc)
        for d in range(1, X):
            send(wo.at[rows], WOX.at[d - 1, rows], "wo", (d, j), xdev(d))

    out_weight(0)

    low = lax.rem(lax.broadcasted_iota(jnp.int32, (TR, hd), 1), hd // 2) < hd // 4

    def turn(raw, gain):
        v = raw.astype(BF16).astype(F32)
        v = v * lax.rsqrt(jnp.mean(v * v, axis=-1, keepdims=True) + EPS) * gain
        other = jnp.where(low, pltpu.roll(v, hd - hd // 4, 1), pltpu.roll(v, hd // 4, 1))
        return (v * cos[...] + other * sin[...]).astype(BF16)

    line_total(AKV, (), lambda k: RKV.at[k], "pkv")
    for j in range(J):
        KV[sp, :, j * hd : (j + 1) * hd] = turn(AKV[:, j * hd : (j + 1) * hd], kg[...])
    KV[sp, :, Kc:] = AKV[:, Kc:].astype(BF16)
    line_own(KV, sp, "kz", ())
    for e in range(1, X):
        send(KV.at[sp], KV.at[sp], "kx", (e, z), xdev(e))

    def kv_hop(n):
        zp = pick(near, n)
        line_hop(zp, KV, zp * X + x, "kz", ())
        for e in range(1, X):
            send(KV.at[zp * X + x], KV.at[zp * X + x], "kx", (e, zp), xdev(e))

    edge = jnp.logical_or(z == 0, z == Z - 1)

    def run_steps():
        for step in q_steps:
            q_step(*step)

    pl.when(edge)(run_steps)

    inner = jnp.logical_not(edge)
    kv_hop(0)
    kv_hop(1)
    pl.when(inner)(lambda: q_step(*q_steps[0]))
    for n in range(2, Z - 1):
        kv_hop(n)
    for j in range(1, J):
        out_weight(j)
    for step in q_steps[1:]:
        pl.when(inner)(lambda step=step: q_step(*step))
    for k in range(Z):
        for e in range(1, X):
            recv(KV.at[k * X + dn(x, e, X)], "kx", (e, k))

    scale = hd ** (-0.5) * LOG2E
    for j in range(J):
        line_total(AQ.at[j], (j,), lambda k: RQ.at[j, k], "pq")

        def one_head(g, carry):
            here = cols(g, hd)
            q = turn(AQ[j, :, here], qg[...])
            keys = KV[:, :, j * hd : (j + 1) * hd].reshape(Z * X * TR, hd)
            vals = KV[:, :, Kc + j * hd : Kc + (j + 1) * hd].reshape(Z * X * TR, hd)
            s = lax.dot_general(q, keys, (((1,), (1,)), ((), ())), preferred_element_type=F32)
            m = jnp.max(s, axis=-1, keepdims=True)
            p = jnp.exp2((s - m) * scale)
            total = jnp.sum(p, axis=-1, keepdims=True)
            o = dot(p.astype(BF16), vals)
            AT[z, j, :, here] = (o / total).astype(BF16)
            return carry

        lax.fori_loop(0, G, one_head, 0)
        for up_down in ((z, z + 1, above), (Z, z - 1, below)):
            send(AT.at[z, j], AT.at[z, j], "at", (j, up_down[0]), dev(up_down[1], x, y, c), ridx=(j, z), when=up_down[2])

    for d in range(1, X):
        for j in range(J):
            recv(WOX.at[d - 1, j * Gc : (j + 1) * Gc], "wo", (d, j))

    def out_block(zp):
        for e in range(X):
            w = wo if e == 0 else WOX.at[e - 1]
            acc = dot(AT[zp, 0], w[:Gc])
            for j in range(1, J):
                acc = acc + dot(AT[zp, j], w[j * Gc : (j + 1) * Gc])
            MB[zp, :, :, :, cols(dn(x, e, X), No)] = acc.astype(BF16).reshape(Y, C, R, No)
        for f in range(1, C):
            send(MB.at[zp, :, up(c, f, C)], MC.at[f - 1, zp], "mc", (f, zp), cdev(f))

    def core_block(zp):
        total = MB[zp, :, c].astype(F32)
        for f in range(1, C):
            recv(MC.at[f - 1, zp], "mc", (f, zp))
            total = total + MC[f - 1, zp].astype(F32)
        MS[zp] = total.astype(BF16)
        for e in range(1, Y):
            send(MS.at[zp, up(y, e, Y)], MY.at[e - 1, zp], "my", (e, zp), ydev(e))

    def row_block(zp, n):
        total = MS[zp, y].astype(F32)
        for e in range(1, Y):
            recv(MY.at[e - 1, zp], "my", (e, zp))
            total = total + MY[e - 1, zp].astype(F32)
        if n == 0:
            FB[z] = total.astype(BF16)
        else:
            FS[n - 1] = total.astype(BF16)
            send(FS.at[n - 1], FB.at[z], "ft", (n,), dev(zp, x, y, c), ridx=(z,))

    blocks = [z] + [pick(near, n) for n in range(Z - 1)]
    for n in range(Z + 2):
        if n < Z:
            zp = blocks[n]
            if n:
                for j in range(J):
                    blk = AT.at[zp, j]
                    recv(blk, "at", (j, zp))
                    onward = jnp.where(zp < z, Z - 1 - z, z) > 0
                    step = jnp.where(zp < z, 1, -1)
                    send(blk, blk, "at", (j, zp), dev(z + step, x, y, c), when=onward)
            out_block(zp)
        if 1 <= n <= Z:
            core_block(blocks[n - 1])
        if n >= 2:
            row_block(blocks[n - 2], n - 2)
    for n in range(1, Z):
        recv(FB.at[blocks[n]], "ft", (blocks[n],))

    square = jnp.zeros((R, 1), F32)
    for k in range(Z):
        v = FB[k].astype(F32)
        square = square + jnp.sum(v * v, axis=-1, keepdims=True)
    inv = lax.rsqrt(square * (1.0 / D) + EPS)
    for k in range(Z):
        part = slice(k * X * No, (k + 1) * X * No)
        out[:, part] = (FB[k].astype(F32) * inv * og[:, part]).astype(BF16)
    for n in range(Z - 1):
        for h in range(H):
            rows = slice(h * TR // H, (h + 1) * TR // H)
            sent.append((wait_for(PKV.at[n, rows], "pkv", (n, h)), None))
            for j in range(J):
                sent.append((wait_for(PQ.at[j, n, rows], "pq", (j, n, h)), None))
    for wait, when in sent:
        if when is None:
            wait()
        else:
            pl.when(when)(wait)


def split_axis(n):
    return 2 if n % 2 == 0 else 1


def fused_plan(n_sp, n_tp, tokens, q_weight, k_weight, o_weight, hd):
    X, C = split_axis(n_sp), split_axis(n_tp)
    Z, Y = n_sp // X, n_tp // C
    R, D = tokens.shape
    Kx, Qc = q_weight.shape
    Kc = k_weight.shape[1]
    J, G = Kc // hd, Qc // Kc
    Gc, TR, No = G * hd, n_tp * R, o_weight.shape[1]
    NX = X * No
    V = pltpu.VMEM
    scratch = [
        ((Z, n_tp, R, Kx * X), BF16),
        ((X - 1, J, Kx, Gc), BF16),
        ((X - 1, Kx, Kc), BF16),
        ((X - 1, Kx, Kc), BF16),
        ((X - 1, Qc, No), BF16),
        ((Z - 1, TR, 2 * Kc), BF16),
        ((Z + 1, TR, 2 * Kc), BF16),
        ((TR, 2 * Kc), F32),
        ((J, Z - 1, TR, Gc), BF16),
        ((J, Z + 1, TR, Gc), BF16),
        ((J, TR, Gc), F32),
        ((n_sp, TR, 2 * Kc), BF16),
        ((Z, J, TR, Gc), BF16),
        ((Z, Y, C, R, NX), BF16),
        ((C - 1, Z, Y, R, NX), BF16),
        ((Z, Y, R, NX), BF16),
        ((Y - 1, Z, R, NX), BF16),
        ((Z - 1, R, NX), BF16),
        ((Z, R, NX), BF16),
    ]
    size = 0
    for shape, kind in scratch:
        n = jnp.dtype(kind).itemsize
        for k in shape:
            n *= k
        size += n
    fits = min(Z, X, Y, C) > 1 and size + TR * n_sp * TR * 12 < 44 * 2**20
    return fits, (Z, X, Y, C, J, G, hd), [V(s, k) for s, k in scratch]


def fused_device(n_sp, n_tp, tokens, q_weight, k_weight, v_weight, o_weight, q_gain, k_gain, out_gain):
    hd = q_gain.shape[0]
    fits, dims, scratch = fused_plan(n_sp, n_tp, tokens, q_weight, k_weight, o_weight, hd)
    if not fits:
        return on_device(tokens, q_weight, k_weight, v_weight, o_weight, q_gain, k_gain, out_gain)
    rows = n_tp * tokens.shape[0]
    positions = lax.axis_index("sp") * rows + lax.iota(jnp.int32, rows)
    cosine, sine = tables(positions, hd)
    low = (jnp.arange(hd) % (hd // 2)) < hd // 4
    sine = jnp.where(low[None, :], -sine, sine)
    Z, X, Y, C, J = dims[:5]
    shapes = sem_shapes(Z, X, Y, C, J)
    names = list(shapes)
    for n in names:
        scratch += [pltpu.SemaphoreType.DMA(shapes[n]), pltpu.SemaphoreType.DMA(shapes[n])]
    spec = pl.BlockSpec(memory_space=pltpu.VMEM)
    return pl.pallas_call(
        functools.partial(fused_kernel, *dims, names),
        out_shape=jax.ShapeDtypeStruct(tokens.shape, BF16),
        in_specs=[spec] * 10,
        out_specs=spec,
        scratch_shapes=scratch,
        compiler_params=pltpu.CompilerParams(
            collective_id=0, has_side_effects=True, vmem_limit_bytes=60 * 2**20
        ),
    )(
        tokens, q_weight, k_weight, v_weight, o_weight,
        q_gain[None, :], k_gain[None, :], out_gain[None, :], cosine, sine,
    )


def solution(mesh):
    placed = (
        P(("sp", "tp"), None),
        P("sp", "tp"),
        P("sp", "tp"),
        P("sp", "tp"),
        P("tp", "sp"),
        P(),
        P(),
        P(),
    )
    return jax.shard_map(
        functools.partial(fused_device, mesh.shape["sp"], mesh.shape["tp"]),
        mesh=mesh, in_specs=placed, out_specs=P(("sp", "tp"), None), check_vma=False,
    )
```
